256 devices in a mesh: sp: 16 (over y, x), tp: 16 (over z, core).
Axes of the slice: x: 4, y: 4, z: 8, core: 2. Of those that a mesh axis runs over, the one named last changes fastest.
Arguments:
- gate_b: bfloat16 [8192, 1024], P('sp', 'tp'), may hold values from -6 to 6
- gate_c: bfloat16 [8192, 1024], P('sp', 'tp'), may hold values from -6 to 6
- values_in: bfloat16 [8192, 1024], P('sp', 'tp'), may hold values from -6 to 6
- conv_w: bfloat16 [3, 1024], P(None, 'tp'), may hold values from -3.5 to 3.5
- documents: int32 [8192], P('sp'), may hold values from 0 to 8, never falling along the last dimension, each value on 1 to 4096 neighbouring positions
- w_out: bfloat16 [1024, 2048], replicated, may hold values from -0.1875 to 0.1875
- resid: bfloat16 [8192, 2048], P(('sp', 'tp')), may hold values from -6 to 6
- norm_gain: bfloat16 [2048], replicated, may hold values from 0.099609375 to 1.8984375
- route_ids: int32 [8192, 2], P(('sp', 'tp')), may hold values from 0 to 15, all different within a row; in each aligned block of 32 rows (0 to 31, 32 to 63, ...) at most 8 rows name the same one
- route_weight: float32 [8192, 2], P(('sp', 'tp')), may hold values from 0.2 to 1
- w_gate: bfloat16 [16, 2048, 7168], P('sp', None, 'tp'), may hold values from -0.125 to 0.125
- w_up: bfloat16 [16, 2048, 7168], P('sp', None, 'tp'), may hold values from -0.125 to 0.125
- w_down: bfloat16 [16, 7168, 2048], P('sp', 'tp'), may hold values from -0.0625 to 0.0625
Outputs:
- layer_out: bfloat16 [8192, 2048], P(('sp', 'tp'))
The draws below stay inside these ranges and needn't reach their ends.
Inputs may be any that keep to these rules, and one draw needn't show every extreme that they name: `route_ids`: each token names two different experts; in the rows of one device no expert is named by more than 8 rows, a bound that some block reaches. `documents`: document numbers never fall along the positions; a document has at most 8192 // 2 positions.
All inputs are finite; a program needn't handle non-finite values.
Results may differ from the reference program's by a relative error of at most 0.018.
Values may be sent and summed in bfloat16 or wider, within the bound.
No kernel may reach another device: no remote copies, remote signals or barrier semaphores. Data moves between devices by JAX's collectives and lax.ppermute only.
A program may use at most 128 MiB of HBM per device.

```python
import math
import jax
import jax.numpy as jnp
import numpy as np
from jax import lax

D = 2048
CH = 1024
FF_E = 7168
KW = 3
TOKENS = 8192
ROWS = 32
EXPERTS = 16
CAP = 8
N_SP = 16
N_TP = 16


def shard_levels(key, extent, cuts, least, high):
    gain, own = 1.0, jax.random.fold_in(key, 6)
    for dim, shards_of in cuts:
        draws = jnp.exp(jax.random.uniform(jax.random.fold_in(own, dim), (shards_of,), jnp.float32, least / len(cuts), high / len(cuts)))
        gain = gain * jnp.repeat(draws, extent[dim] // shards_of).reshape([-1 if axis == dim else 1 for axis in range(len(extent))])
    return gain


def profile(number_of, total, bound, skew):
    portions = [(1 << 20) // math.isqrt(rank ** skew) + 1 for rank in range(2, number_of + 1)]
    surplus, counts = total - bound - (number_of - 1), [1] * (number_of - 1)
    while surplus > 0:
        candidates = [i for i in range(number_of - 1) if counts[i] < bound]
        mass, left = sum([portions[i] for i in candidates]), surplus
        for i in candidates:
            addition = min(bound - counts[i], max(1, left * portions[i] // mass), surplus)
            counts[i] = counts[i] + addition
            surplus = surplus - addition
    return np.array([bound] + counts)


def ragged_sizes(stream_key, amount, total, limit, skew):
    if amount == 2:
        one = jax.random.randint(stream_key, (), max(1, total - limit), min(limit, total - 1) + 1)
        return jnp.stack([one, total - one])
    lengths = jnp.asarray(profile(amount, total, limit, skew), jnp.int32)
    couples = (amount - 1) // 2
    giver, sink = lengths[1:1 + 2 * couples:2], lengths[2:2 + 2 * couples:2]
    slack = jnp.minimum(giver - 1, limit - sink)
    moved = jax.random.randint(jax.random.fold_in(stream_key, 1), (couples,), 0, 1 << 20) % (slack + 1)
    lengths = lengths.at[1:1 + 2 * couples:2].set(giver - moved).at[2:2 + 2 * couples:2].set(sink + moved)
    return lengths[jax.random.permutation(jax.random.fold_in(stream_key, 2), amount)]


def assign_block(own_key, own, number, rows, number_of, top, limit, skew):
    order = jax.random.permutation(own_key, number_of)
    crowded, common = shares(number_of, rows * top, limit, skew, True), shares(number_of, rows * top, limit, skew, False)
    places = jnp.arange(number_of)

    def named(lengths, rotation):
        used = int((lengths > 0).sum())
        fixed = max(1, used // 4)
        shifted = fixed + (places - fixed + rotation * (used - fixed)) % max(1, number_of - fixed)
        return jnp.zeros((number_of,), jnp.int32).at[order[jnp.where(places < fixed, places, shifted)]].set(jnp.asarray(lengths, jnp.int32))

    lengths = jnp.where(number % 4 == 0, named(crowded, number // 4), named(common, number - number // 4 - 1))
    mixed = jax.random.permutation(jax.random.fold_in(own, 3), number_of)
    giver, receiver = mixed[0:number_of // 2 * 2:2], mixed[1:number_of // 2 * 2:2]
    slack = jnp.minimum(lengths[giver] - 1, limit - lengths[receiver]) // 2
    slack = jnp.where((giver == order[0]) | (receiver == order[0]) | (lengths[receiver] == 0), 0, jnp.maximum(slack, 0))
    shifted = jax.random.randint(jax.random.fold_in(own, 4), (number_of // 2,), 0, 1 << 20) % (slack + 1)
    lengths = lengths.at[giver].add(-shifted).at[receiver].add(shifted)
    items = jnp.searchsorted(jnp.cumsum(lengths), jnp.arange(rows * top), side="right").astype(jnp.int32)
    listing = items.reshape(top, rows).T
    listing = listing[jax.random.permutation(jax.random.fold_in(own, 1), rows)]
    rotation = jax.random.randint(jax.random.fold_in(own, 2), (rows, 1), 0, top)
    return jnp.take_along_axis(listing, (jnp.arange(top)[None, :] + rotation) % top, axis=1)


def shares(count, total, bound, lean, full):
    loads = [(1 << 20) // math.isqrt(grade ** lean) + 1 for grade in range(1, count + 1)]
    largest = bound if full else min(bound, max(-(-total // count), total * loads[0] // sum(loads)))
    least = 1 if total - largest >= count - 1 else 0
    counts, spare = [largest] + [least] * (count - 1), total - largest - least * (count - 1)
    while spare > 0:
        movable = [i for i in range(1, count) if counts[i] < largest] or [i for i in range(1, count) if counts[i] < bound]
        mass, remaining = sum([loads[i] for i in movable]), spare
        for i in movable:
            addition = min(bound - counts[i], max(1, remaining * loads[i] // mass), spare)
            counts[i] = counts[i] + addition
            spare = spare - addition
    return np.array(counts)


def centred(stream_key, dims, deviation, most, cuts=(), held_as=jnp.bfloat16):
    factor_of = shard_levels(stream_key, dims, cuts, -0.22, 0.18) if cuts else 1.0
    result = jax.random.normal(stream_key, dims, jnp.float32) * deviation * factor_of
    return jnp.minimum(jnp.maximum(result, -most), most).astype(held_as)


def setup_inputs(seed: int = 0) -> dict:
    arg_keys = jax.random.split(jax.random.key(seed), 14)
    gate_b = centred(arg_keys[0], (TOKENS, CH), 1.0, 6.0, ((0, 16), (1, 16)))
    gate_c = centred(arg_keys[1], (TOKENS, CH), 1.0, 6.0, ((0, 16), (1, 16)))
    values_in = centred(arg_keys[2], (TOKENS, CH), 1.0, 6.0, ((0, 16), (1, 16)))
    conv_w = centred(arg_keys[3], (KW, CH), KW ** -0.5, 3.5, ((1, 16),))
    documents = jnp.searchsorted(jnp.cumsum(ragged_sizes(arg_keys[4], N_SP // 2 + 1, TOKENS, TOKENS // 2, 1)), jnp.arange(TOKENS), side="right").astype(jnp.int32)
    w_out = centred(arg_keys[5], (CH, D), CH ** -0.5, 0.1875)
    resid = centred(arg_keys[6], (TOKENS, D), 1.0, 6.0, ((0, 256),))
    norm_gain = jnp.clip(1.0 + 0.18 * jax.random.normal(arg_keys[7], (D,), jnp.float32), 0.099609375, 1.8984375).astype(jnp.bfloat16)
    route_ids_keys = jax.random.split(jax.random.fold_in(arg_keys[8], 1), TOKENS // ROWS)
    route_ids_turns = jax.random.permutation(jax.random.fold_in(arg_keys[8], 3), TOKENS // ROWS)
    route_ids = jax.vmap(lambda own, number: assign_block(jax.random.fold_in(arg_keys[8], 2), own, number, ROWS, EXPERTS, 2, CAP, 2))(route_ids_keys, route_ids_turns).reshape((TOKENS, 2))
    route_weight = jnp.clip(0.2 + 0.8 * jax.random.uniform(arg_keys[9], (TOKENS, 2), jnp.float32) ** shard_levels(arg_keys[9], (TOKENS, 2), ((0, 256),), -0.2, 0.2), 0.2, 1.0)
    w_gate = centred(arg_keys[10], (EXPERTS, D, FF_E), D ** -0.5, 0.125, ((0, 16), (2, 16)))
    w_up = centred(arg_keys[11], (EXPERTS, D, FF_E), D ** -0.5, 0.125, ((0, 16), (2, 16)))
    w_down = centred(arg_keys[12], (EXPERTS, FF_E, D), FF_E ** -0.5, 0.0625, ((0, 16), (1, 16)))
    return {"gate_b": gate_b, "gate_c": gate_c, "values_in": values_in, "conv_w": conv_w, "documents": documents, "w_out": w_out, "resid": resid, "norm_gain": norm_gain, "route_ids": route_ids, "route_weight": route_weight, "w_gate": w_gate, "w_up": w_up, "w_down": w_down}


def reference(gate_b, gate_c, values_in, conv_w, documents, w_out, resid, norm_gain, route_ids, route_weight, w_gate, w_up, w_down):
    product = gate_c.astype(jnp.float32) * values_in.astype(jnp.float32)
    padded = jnp.concatenate([jnp.zeros((2, CH), jnp.float32), product], axis=0)
    padded_docs = jnp.concatenate([jnp.full((2,), -1, jnp.int32), documents], axis=0)
    kernel_taps = conv_w.astype(jnp.float32)
    near_mask = (padded_docs[1:-1] == documents).astype(jnp.float32)[:, None]
    far_mask = (padded_docs[:-2] == documents).astype(jnp.float32)[:, None]
    convolved = kernel_taps[2] * product + kernel_taps[1] * padded[1:-1] * near_mask + kernel_taps[0] * padded[:-2] * far_mask
    mixed_rows = (gate_b.astype(jnp.float32) * convolved).astype(jnp.bfloat16)
    projected = jnp.dot(mixed_rows, w_out, preferred_element_type=jnp.float32)
    hidden_state = (resid.astype(jnp.float32) + projected).astype(jnp.bfloat16)
    state_wide = hidden_state.astype(jnp.float32)
    normed = (state_wide * lax.rsqrt(lax.optimization_barrier(jnp.mean(state_wide * state_wide, axis=-1, keepdims=True)) + 1e-06) * norm_gain.astype(jnp.float32)).astype(jnp.bfloat16)
    blocks = TOKENS // ROWS
    block_ids = route_ids.reshape(blocks, 2 * ROWS)
    one_hot = (block_ids[:, :, None] == jnp.arange(EXPERTS, dtype=jnp.int32)[None, None, :]).astype(jnp.int32)
    rank_in = lax.optimization_barrier(jnp.sum((jnp.cumsum(one_hot, axis=1) - one_hot) * one_hot, axis=2))
    per_expert = blocks * CAP
    block_index = jnp.arange(blocks, dtype=jnp.int32)[:, None]
    flat_slot = (block_ids * per_expert + block_index * CAP + rank_in).astype(jnp.int32)
    token_index = (block_index * ROWS + jnp.arange(2 * ROWS, dtype=jnp.int32)[None, :] // 2).astype(jnp.int32)
    slot_table = jnp.full((EXPERTS * per_expert,), TOKENS, jnp.int32).at[flat_slot.reshape(-1)].set(token_index.reshape(-1))
    padded_rows = jnp.concatenate([normed, jnp.zeros((1, D), jnp.bfloat16)], axis=0)

    def serve_expert(operands):
        slot_rows, gate_weight, up_weight, down_weight = operands
        chosen = padded_rows[slot_rows]
        gate_part = jnp.dot(chosen, gate_weight, preferred_element_type=jnp.float32)
        up_part = jnp.dot(chosen, up_weight, preferred_element_type=jnp.float32)
        activated = (jax.nn.silu(gate_part) * up_part).astype(jnp.bfloat16)
        pieces = jnp.einsum('snf,nfd->snd', activated.reshape(per_expert, N_TP, FF_E // N_TP).astype(jnp.float32), down_weight.reshape(N_TP, FF_E // N_TP, D).astype(jnp.float32))
        rounded = lax.optimization_barrier(pieces.astype(jnp.bfloat16))
        return lax.optimization_barrier(jnp.sum(rounded.astype(jnp.float32), axis=1)).astype(jnp.bfloat16)
    expert_out = lax.map(serve_expert, (slot_table.reshape(EXPERTS, per_expert), w_gate, w_up, w_down))
    picked = expert_out.reshape(EXPERTS * per_expert, D)[flat_slot.reshape(TOKENS, 2)]
    combined = lax.optimization_barrier(jnp.sum(route_weight[:, :, None].astype(jnp.float32) * picked.astype(jnp.float32), axis=1))
    return (hidden_state.astype(jnp.float32) + combined).astype(jnp.bfloat16)
```

```python
import functools

import jax
import jax.numpy as jnp
from jax import lax
from jax.experimental import pallas as pl
from jax.experimental.pallas import tpu as pltpu
from jax.sharding import Mesh, PartitionSpec as P

CHUNKS = 2


def passed_along(block, axis, distance):
    devices = range(lax.axis_size(axis))
    route = [(i - distance, i) for i in devices if i - distance in devices]
    return lax.ppermute(block, axis, route)


def around(block, step):
    size = lax.axis_size("z")
    return lax.ppermute(block, "z", [(i, (i + step) % size) for i in range(size)])


def swapped(block):
    return lax.ppermute(block, "core", [(0, 1), (1, 0)])


def expert_kernel(count, *refs):
    rows_in, weights = refs[:count], refs[count : count + 6]
    rows_out, (rows, activated) = refs[count + 6 : 2 * count + 6], refs[2 * count + 6 :]
    gates, ups, downs = weights[0:2], weights[2:4], weights[4:6]
    each = rows_in[0].shape[0]
    width = activated.shape[2]
    for i in range(count):
        rows[i * each : (i + 1) * each, :] = rows_in[i][...]
    contract_minor = (((1,), (1,)), ((), ()))

    for half in range(2):

        def hidden(chunk, carry, half=half):
            units = pl.ds(pl.multiple_of(chunk * width, width), width)
            gate = lax.dot_general(
                rows[...], gates[half][units, :], contract_minor, preferred_element_type=jnp.float32
            )
            up = lax.dot_general(
                rows[...], ups[half][units, :], contract_minor, preferred_element_type=jnp.float32
            )
            activated[half * CHUNKS + chunk] = (gate * jax.nn.sigmoid(gate) * up).astype(jnp.bfloat16)
            return carry

        lax.fori_loop(0, CHUNKS, hidden, 0)

    tile = 256

    def project(n, carry):
        columns = pl.ds(pl.multiple_of(n * tile, tile), tile)
        total = None
        for half in range(2):
            for chunk in range(CHUNKS):
                term = jnp.dot(
                    activated[half * CHUNKS + chunk],
                    downs[half][chunk * width : (chunk + 1) * width, columns],
                    preferred_element_type=jnp.float32,
                )
                total = term if total is None else total + term
        for i in range(count):
            rows_out[i][:, columns] = total[i * each : (i + 1) * each].astype(jnp.bfloat16)
        return carry

    lax.fori_loop(0, downs[0].shape[1] // tile, project, 0)


def expert(blocks, weights):
    count, (each, model) = len(blocks), blocks[0].shape
    units = weights[0].shape[0]
    flops = 2 * 3 * count * each * model * 2 * units
    moved = 2 * (6 * units * model + 2 * count * each * model)
    return pl.pallas_call(
        functools.partial(expert_kernel, count),
        out_shape=[jax.ShapeDtypeStruct((each, model), jnp.bfloat16)] * count,
        in_specs=[pl.BlockSpec(memory_space=pltpu.VMEM)] * (count + 6),
        out_specs=[pl.BlockSpec(memory_space=pltpu.VMEM)] * count,
        scratch_shapes=[
            pltpu.VMEM((count * each, model), jnp.bfloat16),
            pltpu.VMEM((2 * CHUNKS, count * each, units // CHUNKS), jnp.bfloat16),
        ],
        compiler_params=pltpu.CompilerParams(vmem_limit_bytes=24 * 1024 * 1024),
        cost_estimate=pl.CostEstimate(flops=flops, bytes_accessed=moved, transcendentals=0),
    )(*blocks, *weights)


def plus(a, b):
    return (a.astype(jnp.float32) + b.astype(jnp.float32)).astype(jnp.bfloat16)


def routed(own, weights):
    half = own.shape[0] // 2
    low = [own]
    high = [own]
    outs = {}
    low.append(around(own, 1))
    high.append(around(own, -1))
    (outs[0],) = expert([own], weights)
    for step in (2, 3):
        low.append(around(low[-1], 1))
        high.append(around(high[-1], -1))
        outs[1 - step], outs[step - 1] = expert([low[step - 1], high[step - 1]], weights)
    far_top = around(low[3][:half], 1)
    far_bottom = around(high[3][half:], -1)
    outs[-3], outs[3] = expert([low[3], high[3]], weights)
    top, bottom = expert([far_top, far_bottom], weights)
    up = around(top, 1)
    down = around(bottom, -1)
    up = around(jnp.concatenate([plus(outs[3][:half], up), outs[3][half:]]), 1)
    down = around(jnp.concatenate([outs[-3][:half], plus(outs[-3][half:], down)]), -1)
    for step in (2, 1):
        up = around(plus(outs[step], up), 1)
        down = around(plus(outs[-step], down), -1)
    return (
        outs[0].astype(jnp.float32) + up.astype(jnp.float32) + down.astype(jnp.float32)
    ).astype(jnp.bfloat16)


def local(
    gate_b,
    gate_c,
    values_in,
    conv_w,
    documents,
    w_out,
    resid,
    norm_gain,
    route_ids,
    route_weight,
    w_gate,
    w_up,
    w_down,
):
    own_weights = [jnp.swapaxes(w_gate[0], 0, 1), jnp.swapaxes(w_up[0], 0, 1), w_down[0]]
    weights = []
    for w in own_weights:
        weights += [w, swapped(w)]
    seq_rows = gate_b.shape[0]
    local_rows = resid.shape[0]
    model_width = resid.shape[1]
    last_rows = jnp.stack([gate_c[seq_rows - 2 :], values_in[seq_rows - 2 :]])
    before, before_docs = passed_along((last_rows, documents[seq_rows - 2 :]), "sp", 1)
    products = jnp.concatenate(
        [
            before[0].astype(jnp.float32) * before[1].astype(jnp.float32),
            gate_c.astype(jnp.float32) * values_in.astype(jnp.float32),
        ],
        axis=0,
    )
    docs_all = jnp.concatenate([before_docs, documents], axis=0)
    kernel_taps = conv_w.astype(jnp.float32)
    near_mask = (docs_all[1:-1] == documents).astype(jnp.float32)[:, None]
    far_mask = (docs_all[:-2] == documents).astype(jnp.float32)[:, None]
    convolved = (
        kernel_taps[2] * products[2:]
        + kernel_taps[1] * products[1:-1] * near_mask
        + kernel_taps[0] * products[:-2] * far_mask
    )
    mixed_rows = (gate_b.astype(jnp.float32) * convolved).astype(jnp.bfloat16)
    token_rows = lax.all_to_all(mixed_rows, ("z", "core"), split_axis=0, concat_axis=1, tiled=True)
    projected = jnp.dot(token_rows, w_out, preferred_element_type=jnp.float32)
    hidden_state = (resid.astype(jnp.float32) + projected).astype(jnp.bfloat16)
    state_wide = hidden_state.astype(jnp.float32)
    normed = (
        state_wide
        * lax.rsqrt(jnp.mean(state_wide * state_wide, axis=-1, keepdims=True) + 1e-06)
        * norm_gain.astype(jnp.float32)
    ).astype(jnp.bfloat16)
    experts = lax.axis_size("sp") * w_gate.shape[0]
    capacity = 4 * local_rows // experts
    flat_ids = route_ids.reshape(-1)
    one_hot = (flat_ids[:, None] == jnp.arange(experts, dtype=jnp.int32)[None, :]).astype(jnp.int32)
    rank_in = jnp.sum((jnp.cumsum(one_hot, axis=0) - one_hot) * one_hot, axis=1)
    slot_index = flat_ids * capacity + rank_in
    placement = (
        slot_index[:, None] == jnp.arange(experts * capacity, dtype=jnp.int32)[None, :]
    ).astype(jnp.bfloat16)
    repeated = jnp.repeat(normed, 2, axis=0)
    dispatch = jnp.einsum(
        "js,jd->sd", placement, repeated, preferred_element_type=jnp.float32
    ).astype(jnp.bfloat16)
    dispatch = dispatch.reshape(experts, capacity, model_width)
    arrived = lax.all_to_all(dispatch, "sp", split_axis=0, concat_axis=0, tiled=True)
    summed = routed(arrived.reshape(experts * capacity, model_width), weights)
    returned = lax.all_to_all(
        summed.reshape(experts, capacity, model_width), "sp", split_axis=0, concat_axis=0, tiled=True
    )
    picked = jnp.take(
        returned.reshape(experts * capacity, model_width), slot_index, axis=0
    ).reshape(local_rows, 2, model_width)
    combined = jnp.sum(route_weight[:, :, None] * picked.astype(jnp.float32), axis=1)
    return (hidden_state.astype(jnp.float32) + combined).astype(jnp.bfloat16)


def solution(mesh):
    cells = Mesh(mesh.devices.reshape(mesh.shape["sp"], -1, 2), ("sp", "z", "core"))
    tp = ("z", "core")
    every = ("sp", "z", "core")
    return jax.shard_map(
        local,
        mesh=cells,
        in_specs=(
            P("sp", tp),
            P("sp", tp),
            P("sp", tp),
            P(None, tp),
            P("sp"),
            P(),
            P(every, None),
            P(),
            P(every, None),
            P(every, None),
            P("sp", None, tp),
            P("sp", None, tp),
            P("sp", tp, None),
        ),
        out_specs=P(every, None),
        check_vma=False,
    )
```

```python
import functools

import jax
import jax.numpy as jnp
from jax import lax
from jax.experimental import pallas as pl
from jax.experimental.pallas import tpu as pltpu
from jax.sharding import Mesh, PartitionSpec as P


LANES = 128
MINOR = (((1,), (1,)), ((), ()))
VMEM = pl.BlockSpec(memory_space=pltpu.VMEM)


def call(kernel, outs, args, flops, scratch=(), limit_mib=16):
    moved = sum(a.size * a.dtype.itemsize for a in (*args, *outs))
    return pl.pallas_call(
        kernel,
        out_shape=list(outs),
        in_specs=[VMEM] * len(args),
        out_specs=[VMEM] * len(outs),
        scratch_shapes=list(scratch),
        compiler_params=pltpu.CompilerParams(vmem_limit_bytes=limit_mib * 1024 * 1024),
        cost_estimate=pl.CostEstimate(flops=flops, bytes_accessed=moved, transcendentals=0),
    )(*args)


def out(shape, dtype=jnp.bfloat16):
    return jax.ShapeDtypeStruct(shape, dtype)


def edge_kernel(gate_ref, value_ref, docs_ref, edge_ref):
    channels, length = gate_ref.shape
    tail = slice(length - LANES, length)
    edge_ref[0:channels, :] = gate_ref[:, tail]
    edge_ref[channels : 2 * channels, :] = value_ref[:, tail]
    docs = docs_ref[docs_ref.shape[0] - 1 :, :].astype(jnp.float32)
    edge_ref[2 * channels :, :] = jnp.broadcast_to(docs, (16, LANES)).astype(jnp.bfloat16)


def conv_kernel(b_ref, c_ref, v_ref, taps_ref, docs_ref, edge_ref, packed_ref):
    channels, length = b_ref.shape
    blocks, half, _ = packed_ref.shape

    def wide(ref):
        return ref.astype(jnp.float32)

    product = wide(c_ref[...]) * wide(v_ref[...])
    edge = wide(edge_ref[...])
    before = edge[0:channels] * edge[channels : 2 * channels]
    every = jnp.concatenate([before, product], axis=1)
    docs_here = jnp.concatenate(
        [wide(docs_ref[i : i + 1, :]) for i in range(docs_ref.shape[0])], axis=1
    )
    docs = jnp.concatenate([edge[2 * channels : 2 * channels + 1], docs_here], axis=1)
    docs = jnp.broadcast_to(docs, (8, docs.shape[1]))
    eye = lax.broadcasted_iota(jnp.int32, (channels, channels), 0) == lax.broadcasted_iota(
        jnp.int32, (channels, channels), 1
    )
    taps = wide(taps_ref[...])

    def tap(k):
        row = jnp.broadcast_to(taps[k : k + 1, :], (channels, channels))
        return jnp.sum(jnp.where(eye, row, 0.0), axis=1, keepdims=True)

    def back(distance):
        near = pltpu.roll(docs, distance, 1)[0:1, LANES:] == docs_here
        return pltpu.roll(every, distance, 1)[:, LANES:], near.astype(jnp.float32)

    one, near = back(1)
    two, far = back(2)
    convolved = tap(2) * product + tap(1) * one * near + tap(0) * two * far
    mixed = wide(b_ref[...]) * convolved
    pair = jnp.concatenate([mixed, pltpu.roll(mixed, length - half, 1)], axis=0).T
    packed_ref[...] = pair.reshape(blocks, 2 * half, 2 * channels)[:, :half].astype(jnp.bfloat16)


def route_kernel(capacity, ids_ref, weights_ref, place_ref, blend_ref):
    slots, tokens = place_ref.shape
    shape = (slots, tokens)
    slot = lax.broadcasted_iota(jnp.int32, shape, 0)
    expert = slot // capacity
    first = jnp.broadcast_to(ids_ref[0:1, :], shape) == expert
    second = jnp.broadcast_to(ids_ref[1:2, :], shape) == expert
    named = (first | second).astype(jnp.float32)
    earlier = lax.broadcasted_iota(jnp.int32, (tokens, tokens), 0) < lax.broadcasted_iota(
        jnp.int32, (tokens, tokens), 1
    )
    rank = jnp.dot(
        named.astype(jnp.bfloat16), earlier.astype(jnp.bfloat16), preferred_element_type=jnp.float32
    )
    here = (named > 0) & (rank.astype(jnp.int32) == slot - expert * capacity)
    place_ref[...] = here.astype(jnp.bfloat16)
    share = jnp.where(
        first,
        jnp.broadcast_to(weights_ref[0:1, :], shape),
        jnp.broadcast_to(weights_ref[1:2, :], shape),
    )
    share = jnp.where(here, share, 0.0)
    share = jnp.concatenate([share, jnp.zeros((slots, LANES - tokens), jnp.float32)], axis=1).T
    rest = share[:tokens]
    for i in range(3):
        term = rest.astype(jnp.bfloat16)
        blend_ref[:, i * slots : (i + 1) * slots] = term
        rest = rest - term.astype(jnp.float32)


def project_kernel(parts_ref, w_ref, resid_ref, gain_ref, place_ref, hidden_ref, sent_ref):
    sources, half, lanes = parts_ref.shape
    channels = lanes // 2
    left = lax.broadcasted_iota(jnp.int32, (half, lanes), 1) < channels
    early, late = [], []
    for i in range(0, sources, 2):
        a = parts_ref[i].astype(jnp.float32)
        b = parts_ref[i + 1].astype(jnp.float32)
        early.append(jnp.where(left, a, pltpu.roll(b, channels, 1)))
        late.append(jnp.where(left, pltpu.roll(a, channels, 1), b))
    rows = jnp.concatenate(
        [jnp.concatenate(early, axis=1), jnp.concatenate(late, axis=1)], axis=0
    ).astype(jnp.bfloat16)
    projected = jnp.dot(rows, w_ref[...], preferred_element_type=jnp.float32)
    hidden = (resid_ref[...].astype(jnp.float32) + projected).astype(jnp.bfloat16)
    hidden_ref[...] = hidden
    wide = hidden.astype(jnp.float32)
    scale = lax.rsqrt(jnp.mean(wide * wide, axis=-1, keepdims=True) + 1e-06)
    normed = (wide * scale * gain_ref[...].astype(jnp.float32)).astype(jnp.bfloat16)
    sent_ref[...] = jnp.dot(
        place_ref[...], normed, preferred_element_type=jnp.float32
    ).astype(jnp.bfloat16)


def combine_kernel(returned_ref, blend_ref, hidden_ref, out_ref):
    slots = returned_ref.shape[0]
    total = None
    for i in range(2, -1, -1):
        term = jnp.dot(
            blend_ref[:, i * slots : (i + 1) * slots],
            returned_ref[...],
            preferred_element_type=jnp.float32,
        )
        total = term if total is None else total + term
    out_ref[...] = (hidden_ref[...].astype(jnp.float32) + total).astype(jnp.bfloat16)


def expert_kernel(count, *refs):
    rows_in, weights = refs[:count], refs[count : count + 6]
    rows_out, (rows, activated) = refs[count + 6 : 2 * count + 6], refs[2 * count + 6 :]
    gates, ups, downs = weights[0:2], weights[2:4], weights[4:6]
    each, model = rows_in[0].shape
    for i in range(count):
        rows[i * each : (i + 1) * each, :] = rows_in[i][...]
    for half in range(2):
        gate = lax.dot_general(gates[half][...], rows[...], MINOR, preferred_element_type=jnp.float32)
        up = lax.dot_general(ups[half][...], rows[...], MINOR, preferred_element_type=jnp.float32)
        value = gate * jax.nn.sigmoid(gate) * up
        activated[half] = value.T.astype(jnp.bfloat16)
    tile = 256

    def project(n, carry):
        columns = pl.ds(pl.multiple_of(n * tile, tile), tile)
        total = jnp.dot(activated[0], downs[0][:, columns], preferred_element_type=jnp.float32)
        total = total + jnp.dot(
            activated[1], downs[1][:, columns], preferred_element_type=jnp.float32
        )
        for i in range(count):
            rows_out[i][:, columns] = total[i * each : (i + 1) * each].astype(jnp.bfloat16)
        return carry

    lax.fori_loop(0, model // tile, project, 0)


def expert(blocks, weights):
    count, (each, model) = len(blocks), blocks[0].shape
    units = weights[0].shape[0]
    return call(
        functools.partial(expert_kernel, count),
        [out((each, model))] * count,
        [*blocks, *weights],
        flops=2 * 3 * count * each * model * 2 * units,
        scratch=[
            pltpu.VMEM((count * each, model), jnp.bfloat16),
            pltpu.VMEM((2, count * each, units), jnp.bfloat16),
        ],
        limit_mib=24,
    )


def around(block, step):
    size = lax.axis_size("z")
    return lax.ppermute(block, "z", [(i, (i + step) % size) for i in range(size)])


def swapped(block):
    return lax.ppermute(block, "core", [(0, 1), (1, 0)])


def plus(a, b):
    return (a.astype(jnp.float32) + b.astype(jnp.float32)).astype(jnp.bfloat16)


UP, DOWN = 1, -1
WAYS = (UP, DOWN)
LEAD = {UP: 0, DOWN: 1}


def routed(own, weights):
    pieces = (0, 1)
    held = {(way, 0, c): own[c] for way in WAYS for c in pieces}
    sums = {}

    def serve(owners):
        sums.update(zip(owners, expert(list(owners.values()), weights)))

    def gather(step, lead):
        for way in WAYS:
            c = LEAD[way] if lead else 1 - LEAD[way]
            held[way, step, c] = around(held[way, step - 1, c], way)

    def came(step, lead):
        blocks = {}
        for way in WAYS:
            c = LEAD[way] if lead else 1 - LEAD[way]
            blocks[-way * step if step < 4 else 4, c] = held[way, step, c]
        return blocks

    gather(1, True)
    gather(1, False)
    serve({(0, c): own[c] for c in pieces})
    for step in (1, 2, 3):
        gather(step + 1, True)
        serve(came(step, True) | (came(step - 1, False) if step > 1 else {}))
        if step < 3:
            gather(step + 1, False)
    serve(came(4, True) | came(3, False))

    running = {}
    for step in (1, 2, 3, 4):
        for lead in (False, True):
            for way in WAYS:
                c = LEAD[way] if lead else 1 - LEAD[way]
                if step == 1 and not lead:
                    continue
                part = sums[4 if step == 1 else way * (5 - step), c]
                if (way, c) in running:
                    part = plus(part, running[way, c])
                running[way, c] = around(part, way)
    total = [
        sums[0, c].astype(jnp.float32)
        + running[UP, c].astype(jnp.float32)
        + running[DOWN, c].astype(jnp.float32)
        for c in pieces
    ]
    return jnp.concatenate(total, axis=0).astype(jnp.bfloat16)


def local(
    gate_b,
    gate_c,
    values_in,
    conv_w,
    documents,
    w_out,
    resid,
    norm_gain,
    route_ids,
    route_weight,
    w_gate,
    w_up,
    w_down,
):
    own_weights = [w_gate[0].T, w_up[0].T, w_down[0]]
    seq_rows, channels = gate_b.shape
    rows, model = resid.shape
    columns = lax.axis_size("sp")
    capacity = 4 * rows // columns
    slots = columns * capacity
    splits = seq_rows // rows

    docs = documents.reshape(-1, LANES)
    (edge,) = call(
        edge_kernel, [out((2 * channels + 16, LANES))], [gate_c.T, values_in.T, docs], flops=1000
    )
    before = lax.ppermute(edge, "sp", [(i, i + 1) for i in range(columns - 1)])
    place, blend = call(
        functools.partial(route_kernel, capacity),
        [out((slots, rows)), out((rows, 3 * slots))],
        [route_ids.T, route_weight.T],
        flops=10_000_000,
    )
    (packed,) = call(
        conv_kernel,
        [out((splits, rows // 2, 2 * channels))],
        [gate_b.T, gate_c.T, values_in.T, conv_w, docs, before],
        flops=10_000_000,
    )
    parts = lax.all_to_all(packed, ("z", "core"), split_axis=0, concat_axis=0, tiled=True)
    hidden, sent = call(
        project_kernel,
        [out((rows, model)), out((slots, model))],
        [parts, w_out, resid, norm_gain.reshape(1, model), place],
        flops=2_000_000_000,
    )
    others = [swapped(w) for w in own_weights]
    sent, *others = lax.optimization_barrier((sent, *others))
    weights = [w for pair in zip(own_weights, others) for w in pair]
    arrived = lax.all_to_all(
        sent.reshape(columns, capacity, model), "sp", split_axis=0, concat_axis=0, tiled=True
    ).reshape(slots, model)
    summed = routed([arrived[: slots // 2], arrived[slots // 2 :]], weights)
    returned = lax.all_to_all(
        summed.reshape(columns, capacity, model), "sp", split_axis=0, concat_axis=0, tiled=True
    ).reshape(slots, model)
    return call(
        combine_kernel, [out((rows, model))], [returned, blend, hidden], flops=50_000_000
    )[0]


def solution(mesh):
    cells = Mesh(mesh.devices.reshape(mesh.shape["sp"], -1, 2), ("sp", "z", "core"))
    tp = ("z", "core")
    every = ("sp", "z", "core")
    return jax.shard_map(
        local,
        mesh=cells,
        in_specs=(
            P("sp", tp),
            P("sp", tp),
            P("sp", tp),
            P(None, tp),
            P("sp"),
            P(),
            P(every, None),
            P(),
            P(every, None),
            P(every, None),
            P("sp", None, tp),
            P("sp", None, tp),
            P("sp", tp, None),
        ),
        out_specs=P(every, None),
        check_vma=False,
    )
```

```python
import functools

import jax
import jax.numpy as jnp
from jax import lax
from jax.experimental import pallas as pl
from jax.experimental.pallas import tpu as pltpu
from jax.sharding import Mesh, PartitionSpec as P


LANES = 128
MINOR = (((1,), (1,)), ((), ()))
VMEM = pl.BlockSpec(memory_space=pltpu.VMEM)
HBM = pl.BlockSpec(memory_space=pltpu.HBM)


def call(kernel, outs, args, flops, scratch=(), limit_mib=4, far=(), near=()):
    moved = sum(a.size * a.dtype.itemsize for a in (*args, *outs))
    placed = {i: pltpu.HBM for i in far} | {i: pltpu.VMEM for i in near}
    args = [
        pltpu.with_memory_space_constraint(a, placed[i]) if i in placed else a
        for i, a in enumerate(args)
    ]
    return pl.pallas_call(
        kernel,
        out_shape=list(outs),
        in_specs=[HBM if i in far else VMEM for i in range(len(args))],
        out_specs=[VMEM] * len(outs),
        scratch_shapes=list(scratch),
        compiler_params=pltpu.CompilerParams(vmem_limit_bytes=limit_mib * 1024 * 1024),
        cost_estimate=pl.CostEstimate(flops=flops, bytes_accessed=moved, transcendentals=0),
    )(*args)


def out(shape, dtype=jnp.bfloat16):
    return jax.ShapeDtypeStruct(shape, dtype)


def staged(sources, targets, sems):
    copies = [pltpu.make_async_copy(*pair, sems.at[i]) for i, pair in enumerate(zip(sources, targets))]
    for copy in copies:
        copy.start()
    return copies


def edge_kernel(*refs):
    *far, docs_ref, c_ref, v_ref, b_ref, taps_ref, edge_ref, sems = refs
    copies = staged(far, (docs_ref, c_ref, v_ref, b_ref, taps_ref), sems)
    channels, length = c_ref.shape
    tail = slice(length - LANES, length)
    copies[0].wait()
    docs = docs_ref[docs_ref.shape[0] - 1 :, :].astype(jnp.float32)
    edge_ref[2 * channels :, :] = jnp.broadcast_to(docs, (16, LANES)).astype(jnp.bfloat16)
    copies[1].wait()
    edge_ref[0:channels, :] = c_ref[:, tail]
    copies[2].wait()
    edge_ref[channels : 2 * channels, :] = v_ref[:, tail]
    copies[3].wait()
    copies[4].wait()


def conv_kernel(docs_ref, c_ref, v_ref, b_ref, taps_ref, edge_ref, packed_ref):
    channels, length = b_ref.shape
    blocks, half, _ = packed_ref.shape

    def wide(ref):
        return ref.astype(jnp.float32)

    product = wide(c_ref[...]) * wide(v_ref[...])
    edge = wide(edge_ref[...])
    before = edge[0:channels] * edge[channels : 2 * channels]
    every = jnp.concatenate([before, product], axis=1)
    docs_here = jnp.concatenate(
        [wide(docs_ref[i : i + 1, :]) for i in range(docs_ref.shape[0])], axis=1
    )
    docs = jnp.concatenate([edge[2 * channels : 2 * channels + 1], docs_here], axis=1)
    docs = jnp.broadcast_to(docs, (8, docs.shape[1]))
    eye = lax.broadcasted_iota(jnp.int32, (channels, channels), 0) == lax.broadcasted_iota(
        jnp.int32, (channels, channels), 1
    )
    taps = wide(taps_ref[...])

    def tap(k):
        row = jnp.broadcast_to(taps[k : k + 1, :], (channels, channels))
        return jnp.sum(jnp.where(eye, row, 0.0), axis=1, keepdims=True)

    def back(distance):
        near = pltpu.roll(docs, distance, 1)[0:1, LANES:] == docs_here
        return pltpu.roll(every, distance, 1)[:, LANES:], near.astype(jnp.float32)

    one, near = back(1)
    two, far = back(2)
    convolved = tap(2) * product + tap(1) * one * near + tap(0) * two * far
    mixed = wide(b_ref[...]) * convolved
    pair = jnp.concatenate([mixed, pltpu.roll(mixed, length - half, 1)], axis=0).T
    packed_ref[...] = pair.reshape(blocks, 2 * half, 2 * channels)[:, :half].astype(jnp.bfloat16)


def route_kernel(
    capacity, ids_far, weights_far, w_far, resid_far, place_ref, blend_ref, w_ref, resid_ref, *own
):
    ids_ref, weights_ref, sems = own
    copies = staged(
        (ids_far, weights_far, w_far, resid_far), (ids_ref, weights_ref, w_ref, resid_ref), sems
    )
    copies[0].wait()
    copies[1].wait()
    slots, tokens = place_ref.shape
    shape = (slots, tokens)
    slot = lax.broadcasted_iota(jnp.int32, shape, 0)
    expert = slot // capacity
    first = jnp.broadcast_to(ids_ref[0:1, :], shape) == expert
    second = jnp.broadcast_to(ids_ref[1:2, :], shape) == expert
    named = (first | second).astype(jnp.float32)
    earlier = lax.broadcasted_iota(jnp.int32, (tokens, tokens), 0) < lax.broadcasted_iota(
        jnp.int32, (tokens, tokens), 1
    )
    rank = jnp.dot(
        named.astype(jnp.bfloat16), earlier.astype(jnp.bfloat16), preferred_element_type=jnp.float32
    )
    here = (named > 0) & (rank.astype(jnp.int32) == slot - expert * capacity)
    place_ref[...] = here.astype(jnp.bfloat16)
    share = jnp.where(
        first,
        jnp.broadcast_to(weights_ref[0:1, :], shape),
        jnp.broadcast_to(weights_ref[1:2, :], shape),
    )
    share = jnp.where(here, share, 0.0)
    share = jnp.concatenate([share, jnp.zeros((slots, LANES - tokens), jnp.float32)], axis=1).T
    rest = share[:tokens]
    for i in range(3):
        term = rest.astype(jnp.bfloat16)
        blend_ref[:, i * slots : (i + 1) * slots] = term
        rest = rest - term.astype(jnp.float32)
    copies[2].wait()
    copies[3].wait()


def project_kernel(parts_ref, w_ref, resid_ref, gain_ref, place_ref, hidden_ref, sent_ref):
    sources, half, lanes = parts_ref.shape
    channels = lanes // 2
    left = lax.broadcasted_iota(jnp.int32, (half, lanes), 1) < channels
    early, late = [], []
    for i in range(0, sources, 2):
        a = parts_ref[i].astype(jnp.float32)
        b = parts_ref[i + 1].astype(jnp.float32)
        early.append(jnp.where(left, a, pltpu.roll(b, channels, 1)))
        late.append(jnp.where(left, pltpu.roll(a, channels, 1), b))
    rows = jnp.concatenate(
        [jnp.concatenate(early, axis=1), jnp.concatenate(late, axis=1)], axis=0
    ).astype(jnp.bfloat16)
    projected = jnp.dot(rows, w_ref[...], preferred_element_type=jnp.float32)
    hidden = (resid_ref[...].astype(jnp.float32) + projected).astype(jnp.bfloat16)
    hidden_ref[...] = hidden
    wide = hidden.astype(jnp.float32)
    scale = lax.rsqrt(jnp.mean(wide * wide, axis=-1, keepdims=True) + 1e-06)
    gain = jnp.concatenate([gain_ref[i : i + 1, :] for i in range(gain_ref.shape[0])], axis=1)
    normed = (wide * scale * gain.astype(jnp.float32)).astype(jnp.bfloat16)
    sent_ref[...] = jnp.dot(
        place_ref[...], normed, preferred_element_type=jnp.float32
    ).astype(jnp.bfloat16)


def combine_kernel(returned_ref, blend_ref, hidden_ref, out_ref):
    slots = returned_ref.shape[0]
    total = None
    for i in range(2, -1, -1):
        term = jnp.dot(
            blend_ref[:, i * slots : (i + 1) * slots],
            returned_ref[...],
            preferred_element_type=jnp.float32,
        )
        total = term if total is None else total + term
    out_ref[...] = (hidden_ref[...].astype(jnp.float32) + total).astype(jnp.bfloat16)


def expert_kernel(count, *refs):
    rows_in, weights = refs[:count], refs[count : count + 6]
    rows_out, (rows, activated) = refs[count + 6 : 2 * count + 6], refs[2 * count + 6 :]
    gates, ups, downs = weights[0:2], weights[2:4], weights[4:6]
    each, model = rows_in[0].shape
    for i in range(count):
        rows[i * each : (i + 1) * each, :] = rows_in[i][...]
    for half in range(2):
        gate = lax.dot_general(gates[half][...], rows[...], MINOR, preferred_element_type=jnp.float32)
        up = lax.dot_general(ups[half][...], rows[...], MINOR, preferred_element_type=jnp.float32)
        value = gate * jax.nn.sigmoid(gate) * up
        activated[half] = value.T.astype(jnp.bfloat16)
    tile = 256

    def project(n, carry):
        columns = pl.ds(pl.multiple_of(n * tile, tile), tile)
        total = jnp.dot(activated[0], downs[0][:, columns], preferred_element_type=jnp.float32)
        total = total + jnp.dot(
            activated[1], downs[1][:, columns], preferred_element_type=jnp.float32
        )
        for i in range(count):
            rows_out[i][:, columns] = total[i * each : (i + 1) * each].astype(jnp.bfloat16)
        return carry

    lax.fori_loop(0, model // tile, project, 0)


def expert(blocks, weights):
    count, (each, model) = len(blocks), blocks[0].shape
    units = weights[0].shape[0]
    return call(
        functools.partial(expert_kernel, count),
        [out((each, model))] * count,
        [*blocks, *weights],
        flops=2 * 3 * count * each * model * 2 * units,
        scratch=[
            pltpu.VMEM((count * each, model), jnp.bfloat16),
            pltpu.VMEM((2, count * each, units), jnp.bfloat16),
        ],
        limit_mib=16,
        near=range(count, count + 6),
    )


def around(block, step):
    size = lax.axis_size("z")
    return lax.ppermute(block, "z", [(i, (i + step) % size) for i in range(size)])


def swapped(block):
    return lax.ppermute(block, "core", [(0, 1), (1, 0)])


def plus(a, b):
    return (a.astype(jnp.float32) + b.astype(jnp.float32)).astype(jnp.bfloat16)


UP, DOWN = 1, -1
WAYS = (UP, DOWN)
LEAD = {UP: 0, DOWN: 1}


def routed(own, weights):
    pieces = (0, 1)
    held = {(way, 0, c): own[c] for way in WAYS for c in pieces}
    sums = {}

    def serve(owners):
        sums.update(zip(owners, expert(list(owners.values()), weights)))

    def gather(step, lead):
        for way in WAYS:
            c = LEAD[way] if lead else 1 - LEAD[way]
            held[way, step, c] = around(held[way, step - 1, c], way)

    def came(step, lead):
        blocks = {}
        for way in WAYS:
            c = LEAD[way] if lead else 1 - LEAD[way]
            blocks[-way * step if step < 4 else 4, c] = held[way, step, c]
        return blocks

    gather(1, True)
    gather(1, False)
    serve({(0, c): own[c] for c in pieces})
    for step in (1, 2, 3):
        gather(step + 1, True)
        serve(came(step, True) | (came(step - 1, False) if step > 1 else {}))
        if step < 3:
            gather(step + 1, False)
    serve(came(4, True) | came(3, False))

    running = {}
    for step in (1, 2, 3, 4):
        for lead in (False, True):
            for way in WAYS:
                c = LEAD[way] if lead else 1 - LEAD[way]
                if step == 1 and not lead:
                    continue
                part = sums[4 if step == 1 else way * (5 - step), c]
                if (way, c) in running:
                    part = plus(part, running[way, c])
                running[way, c] = around(part, way)
    total = [
        sums[0, c].astype(jnp.float32)
        + running[UP, c].astype(jnp.float32)
        + running[DOWN, c].astype(jnp.float32)
        for c in pieces
    ]
    return jnp.concatenate(total, axis=0).astype(jnp.bfloat16)


def local(
    gate_b,
    gate_c,
    values_in,
    conv_w,
    documents,
    w_out,
    resid,
    norm_gain,
    route_ids,
    route_weight,
    w_gate,
    w_up,
    w_down,
):
    own_weights = [w_gate[0].T, w_up[0].T, w_down[0]]
    seq_rows, channels = gate_b.shape
    rows, model = resid.shape
    columns = lax.axis_size("sp")
    capacity = 4 * rows // columns
    slots = columns * capacity
    splits = seq_rows // rows

    inputs = [documents.reshape(-1, LANES), gate_c.T, values_in.T, gate_b.T, conv_w]
    *inputs, edge = call(
        edge_kernel,
        [*(out(x.shape, x.dtype) for x in inputs), out((2 * channels + 16, LANES))],
        inputs,
        flops=1000,
        far=range(5),
        scratch=[pltpu.SemaphoreType.DMA((5,))],
    )
    before = lax.ppermute(edge, "sp", [(i, i + 1) for i in range(columns - 1)])
    others = []
    for w in own_weights:
        others.append(swapped(w))
    place, blend, w_out, resid = call(
        functools.partial(route_kernel, capacity),
        [
            out((slots, rows)),
            out((rows, 3 * slots)),
            out(w_out.shape, w_out.dtype),
            out(resid.shape, resid.dtype),
        ],
        [route_ids.T, route_weight.T, w_out, resid],
        flops=10_000_000,
        far=range(4),
        scratch=[
            pltpu.VMEM(route_ids.T.shape, route_ids.dtype),
            pltpu.VMEM(route_weight.T.shape, route_weight.dtype),
            pltpu.SemaphoreType.DMA((4,)),
        ],
    )
    (packed,) = call(
        conv_kernel, [out((splits, rows // 2, 2 * channels))], [*inputs, before], flops=10_000_000
    )
    parts = lax.all_to_all(packed, ("z", "core"), split_axis=0, concat_axis=0, tiled=True)
    hidden, sent = call(
        project_kernel,
        [out((rows, model)), out((slots, model))],
        [parts, w_out, resid, norm_gain.reshape(-1, LANES), place],
        flops=2_000_000_000,
    )
    sent, *others = lax.optimization_barrier((sent, *others))
    weights = [w for pair in zip(own_weights, others) for w in pair]
    arrived = lax.all_to_all(
        sent.reshape(columns, capacity, model), "sp", split_axis=0, concat_axis=0, tiled=True
    ).reshape(slots, model)
    summed = routed([arrived[: slots // 2], arrived[slots // 2 :]], weights)
    returned = lax.all_to_all(
        summed.reshape(columns, capacity, model), "sp", split_axis=0, concat_axis=0, tiled=True
    ).reshape(slots, model)
    return call(
        combine_kernel, [out((rows, model))], [returned, blend, hidden], flops=50_000_000
    )[0]


def solution(mesh):
    cells = Mesh(mesh.devices.reshape(mesh.shape["sp"], -1, 2), ("sp", "z", "core"))
    tp = ("z", "core")
    every = ("sp", "z", "core")
    return jax.shard_map(
        local,
        mesh=cells,
        in_specs=(
            P("sp", tp),
            P("sp", tp),
            P("sp", tp),
            P(None, tp),
            P("sp"),
            P(),
            P(every, None),
            P(),
            P(every, None),
            P(every, None),
            P("sp", None, tp),
            P("sp", None, tp),
            P("sp", tp, None),
        ),
        out_specs=P(every, None),
        check_vma=False,
    )
```
